32 devices in a mesh: fs: 8 (over z, x), tp: 4 (over y, core).
Axes of the slice: x: 2, y: 2, z: 4, core: 2. Of those that a mesh axis runs over, the one named last changes fastest.
Arguments:
- tokens: bfloat16 [64, 2048], P(('fs', 'tp')), may hold values from -6 to 6
- route_experts: int32 [64, 2], P(('fs', 'tp')), may hold values from 0 to 3, as said below
- route_logits: float32 [64, 2], P(('fs', 'tp')), may hold values from -8 to 8
- norm_gain: float32 [2048], P('fs'), may hold values from 0.1 to 1.9
- gate_train: float32 [4, 2048, 8192], P(None, 'fs', 'tp'), may hold values from -0.125 to 0.125
- up_train: float32 [4, 2048, 8192], P(None, 'fs', 'tp'), may hold values from -0.125 to 0.125
- down_train: float32 [4, 2048, 8192], P(None, 'fs', 'tp'), may hold values from -0.125 to 0.125
Outputs:
- gate_serve: bfloat16 [8, 2048, 4096], P('fs')
- up_serve: bfloat16 [8, 2048, 4096], P('fs')
- down_serve: bfloat16 [8, 2048, 4096], P('fs')
- mixed: bfloat16 [64, 2048], P(('fs', 'tp'))
The draws below stay inside these ranges and needn't reach their ends.
Inputs may be any that keep to these rules, and one draw needn't show every extreme that they name: `route_experts`: the two experts of a row differ; any expert may be named by every row of the devices that share one index along tp, and in every draw some expert is.
All inputs are finite; a program needn't handle non-finite values.
Results may differ from the reference program's by a relative error of at most 0.0085.
Values may be sent and summed in bfloat16 or wider, within the bound.
A program may use at most 192 MiB of HBM per device.

```python
import jax
import jax.numpy as jnp
from jax import lax

D = 2048
FF = 8192
EXPERTS = 4
TOK_DEV = 2
TOKENS = 64
SLICES = 2
N_TP = 4


def draw_route_experts(key, part):
    keys = jax.random.split(key, 7)
    positions = jnp.arange(TOKENS, dtype=jnp.int32)
    group_index = positions // TOK_DEV % N_TP
    favour = jax.random.randint(keys[0], (N_TP,), 0, EXPERTS, dtype=jnp.int32)
    full_group = jax.random.randint(keys[1], (), 0, N_TP, dtype=jnp.int32)
    share = jax.random.randint(keys[2], (N_TP,), 40, 91, dtype=jnp.int32)
    share = jnp.where(jnp.arange(N_TP, dtype=jnp.int32) == full_group, 100, share)
    picked = jax.random.randint(keys[3], (TOKENS,), 0, 100, dtype=jnp.int32)
    others = jax.random.randint(keys[4], (TOKENS,), 0, EXPERTS, dtype=jnp.int32)
    first = jnp.where(picked < share[group_index], favour[group_index], others)
    offset = jax.random.randint(keys[5], (TOKENS,), 1, EXPERTS, dtype=jnp.int32)
    second = (first + offset) % EXPERTS
    flipped = jax.random.randint(keys[6], (TOKENS,), 0, 2, dtype=jnp.int32)
    column_a = jnp.where(flipped == 1, second, first)
    column_b = jnp.where(flipped == 1, first, second)
    return jnp.stack([column_a, column_b], axis=1).astype(jnp.int32)


def block_scale(stream_key, shape, pieces, low, largest):
    loudness = 1.0
    for position, parts in pieces:
        heights = jax.random.uniform(jax.random.fold_in(jax.random.fold_in(stream_key, 6), position), (parts,), jnp.float32, low / len(pieces), largest / len(pieces))
        loudness = loudness * jnp.repeat(jnp.exp(heights), shape[position] // parts).reshape((-1,) + (1,) * (len(shape) - 1 - position))
    return loudness


def scatter_about(stream_key, dims, scale, most, cuts=(), kind=jnp.bfloat16):
    gain = block_scale(stream_key, dims, cuts, -0.22, 0.18) if cuts else 1.0
    array = jax.random.normal(stream_key, dims, jnp.float32) * scale * gain
    return jnp.minimum(jnp.maximum(array, -most), most).astype(kind)


def setup_inputs(seed: int = 0) -> dict:
    streams_of = jax.random.split(jax.random.key(seed), 8)
    tokens = scatter_about(streams_of[0], (TOKENS, D), 1.0, 6.0, ((0, 32),))
    route_experts = draw_route_experts(jax.random.fold_in(streams_of[7], 71), 0)
    route_logits = scatter_about(streams_of[2], (TOKENS, 2), 2.0, 8.0, ((0, 32),), jnp.float32)
    norm_gain = jnp.clip(1.0 + 0.18 * jax.random.normal(streams_of[3], (D,), jnp.float32), 0.1, 1.9)
    gate_train = scatter_about(streams_of[4], (EXPERTS, D, FF), D ** -0.5, 0.125, ((1, 8), (2, 4)), jnp.float32)
    up_train = scatter_about(streams_of[5], (EXPERTS, D, FF), D ** -0.5, 0.125, ((1, 8), (2, 4)), jnp.float32)
    down_train = scatter_about(streams_of[6], (EXPERTS, D, FF), (FF // 4) ** -0.5, 0.125, ((1, 8), (2, 4)), jnp.float32)
    return {"tokens": tokens, "route_experts": route_experts, "route_logits": route_logits, "norm_gain": norm_gain, "gate_train": gate_train, "up_train": up_train, "down_train": down_train}


def relayout(matrix):
    count, width, hidden = matrix.shape
    blocks = matrix.reshape(count, width, SLICES, hidden // SLICES)
    return blocks.transpose(0, 2, 1, 3).reshape(count * SLICES, width, hidden // SLICES)

def normalize(tokens):
    values = tokens.astype(jnp.float32)
    row_mean = lax.optimization_barrier(jnp.mean(values, axis=-1, keepdims=True))
    centered = values - row_mean
    row_var = lax.optimization_barrier(jnp.mean(centered * centered, axis=-1, keepdims=True))
    return (centered * lax.rsqrt(row_var + 1e-05)).astype(jnp.bfloat16)

def route_table(route_experts, route_logits):
    first = jax.nn.sigmoid(route_logits[:, 0] - route_logits[:, 1])
    second = jax.nn.sigmoid(route_logits[:, 1] - route_logits[:, 0])
    labels = jnp.arange(EXPERTS, dtype=jnp.int32)
    table = first[:, None] * (route_experts[:, 0:1] == labels[None, :]).astype(jnp.float32)
    table = table + second[:, None] * (route_experts[:, 1:2] == labels[None, :]).astype(jnp.float32)
    return table.astype(jnp.bfloat16)

def reference(tokens, route_experts, route_logits, norm_gain, gate_train, up_train, down_train):
    gate_new = (norm_gain[None, :, None] * gate_train).astype(jnp.bfloat16)
    up_new = (norm_gain[None, :, None] * up_train).astype(jnp.bfloat16)
    down_new = down_train.astype(jnp.bfloat16)
    normed = normalize(tokens)
    table = route_table(route_experts, route_logits)
    total = jnp.zeros((tokens.shape[0], tokens.shape[1]), jnp.float32)
    for expert in range(EXPERTS):
        gate_act = jnp.dot(normed, gate_new[expert], preferred_element_type=jnp.float32)
        up_act = jnp.dot(normed, up_new[expert], preferred_element_type=jnp.float32)
        weight = table[:, expert].astype(jnp.float32)[:, None]
        hidden = (weight * jax.nn.silu(gate_act) * up_act).astype(jnp.bfloat16)
        total = total + jnp.dot(hidden, down_new[expert].T, preferred_element_type=jnp.float32)
    return (relayout(gate_new), relayout(up_new), relayout(down_new), total.astype(jnp.bfloat16))
```

```python
import functools

import jax
import jax.numpy as jnp
from jax import lax
from jax.experimental import pallas as pl
from jax.experimental.pallas import tpu as pltpu
from jax.sharding import PartitionSpec as P

MESH = pl.DeviceIdType.MESH
PARTS = 8
LAG_Y = 3
LAG_X = 6
PER_STEP = 2
SLOTS = 4
TILE = 512
VMEM_LIMIT = 16400000
STORES = 4
REDUCE_LIMIT = 2000000
PAD = 128


def for_sending(array):
    return jax.tree.map(lambda a: a.astype(jnp.bfloat16) if a.dtype == jnp.float32 else a, array)


def normalize(tokens):
    values = tokens.astype(jnp.float32)
    row_mean = jnp.mean(values, axis=-1, keepdims=True)
    centered = values - row_mean
    row_var = jnp.mean(centered * centered, axis=-1, keepdims=True)
    return (centered * lax.rsqrt(row_var + 1e-05)).astype(jnp.bfloat16)


def per_device_general(tokens, route_experts, route_logits, norm_gain, gate_train, up_train, down_train):
    fs_size = lax.axis_size("fs")
    tp_size = lax.axis_size("tp")
    expert_count = gate_train.shape[0]
    slices = fs_size // expert_count
    scale = norm_gain[None, :, None]
    gate_half = (scale * gate_train).astype(jnp.bfloat16)
    up_half = (scale * up_train).astype(jnp.bfloat16)
    down_half = down_train.astype(jnp.bfloat16)
    swapped = (
        lax.all_to_all(gate_half, "tp", split_axis=1, concat_axis=2, tiled=True),
        lax.all_to_all(up_half, "tp", split_axis=1, concat_axis=2, tiled=True),
        lax.all_to_all(down_half, "tp", split_axis=1, concat_axis=2, tiled=True),
    )
    quarter = swapped[0].shape[1]
    hidden_total = swapped[0].shape[2]
    block_width = hidden_total // slices

    def split_quarter(matrix):
        blocks = matrix.reshape(expert_count, quarter, slices, block_width)
        return blocks.transpose(0, 2, 1, 3).reshape(expert_count * slices, quarter, block_width)

    owned = lax.all_to_all(
        for_sending(tuple((split_quarter(matrix) for matrix in swapped))),
        "fs",
        split_axis=0,
        concat_axis=1,
        tiled=True,
    )
    stacked = tuple((matrix.reshape(1, fs_size, 1, quarter, block_width) for matrix in owned))
    joined = jax.tree.map(
        lambda part, own: part.astype(own.dtype),
        lax.all_gather(for_sending(stacked), "tp", axis=2, tiled=True),
        stacked,
    )
    gate_serve, up_serve, down_serve = tuple(
        (matrix.reshape(1, fs_size * tp_size * quarter, block_width) for matrix in joined)
    )
    normed = normalize(tokens)
    first = jax.nn.sigmoid(route_logits[:, 0] - route_logits[:, 1])
    second = jax.nn.sigmoid(route_logits[:, 1] - route_logits[:, 0])
    labels = jnp.arange(expert_count, dtype=jnp.int32)
    table = first[:, None] * (route_experts[:, 0:1] == labels[None, :]).astype(jnp.float32)
    table = table + second[:, None] * (route_experts[:, 1:2] == labels[None, :]).astype(jnp.float32)
    table = table.astype(jnp.bfloat16)
    rows_all, table_all = (
        lax.all_gather(normed, "fs", axis=0, tiled=True),
        lax.all_gather(table, "fs", axis=0, tiled=True),
    )
    own_expert = lax.axis_index("fs") // slices
    selector = (labels == own_expert).astype(jnp.float32)
    weight = jnp.sum(table_all.astype(jnp.float32) * selector[None, :], axis=1)
    gate_act = jnp.dot(rows_all, gate_serve[0], preferred_element_type=jnp.float32)
    up_act = jnp.dot(rows_all, up_serve[0], preferred_element_type=jnp.float32)
    hidden = (weight[:, None] * jax.nn.silu(gate_act) * up_act).astype(jnp.bfloat16)
    down_own = down_serve[0]
    summed = lax.psum_scatter(
        lax.dot_general(
            hidden, down_own, (((1,), (1,)), ((), ())), preferred_element_type=jnp.float32
        ),
        "fs",
        scatter_dimension=0,
        tiled=True,
    )
    return (gate_serve, up_serve, down_serve, summed.astype(jnp.bfloat16))


def exchange_kernel(
    tokens_ref, experts_ref, logits_ref, gain_ref, gate_in, up_in, down_in,
    served, transit, part_ref,
    src, staged, scale, all_ref, acts, hidden_ref,
    l_in, z_s, z_r, y_s, y_r, x_s, x_r, c_s, c_r, g_s, g_r
):
    trained = (gate_in, up_in, down_in)
    matrices = len(trained)
    experts, rows, width = gate_in.shape
    fs_size, count, _ = all_ref.shape
    depth = tokens_ref.shape[1]
    chunk = rows // PARTS
    group = matrices * PARTS
    total = experts * group
    half = group // 2
    early = group + half
    f = lax.axis_index("fs")
    t = lax.axis_index("tp")
    z, x = lax.div(f, 2), lax.rem(f, 2)
    s, c = lax.div(t, 2), lax.rem(t, 2)
    y_peer = (f, (1 - s) * 2 + c)
    c_peer = (f, s * 2 + 1 - c)
    x_peer = (z * 2 + 1 - x, t)
    low = z < experts // 2
    outer = (z == 0) | (z == experts - 1)
    near = z + 1 - 2 * lax.rem(z, 2)
    across = jnp.where(low, experts // 2, experts // 2 - 1)
    beyond = jnp.where(low, experts - 1, 0)
    far = (jnp.where(c == 0, across, beyond), jnp.where(c == 0, beyond, across))

    def load(k):
        g, e = lax.div(k, experts), lax.rem(k, experts)
        slot = lax.rem(k, SLOTS)
        row = pl.multiple_of(lax.rem(g, PARTS) * chunk, chunk)
        for m in range(matrices):
            @pl.when(lax.div(g, PARTS) == m)
            def _():
                pltpu.make_async_copy(
                    trained[m].at[e, pl.ds(row, chunk)], staged.at[slot], l_in.at[slot]
                ).start()

    @pl.loop(0, SLOTS)
    def _(k):
        load(k)

    barrier = pltpu.get_barrier_semaphore()
    fs_peers = [(lax.rem(f + q, fs_size), t) for q in range(1, fs_size)]
    for peer in (*fs_peers, y_peer, c_peer):
        pl.semaphore_signal(barrier, inc=1, device_id=peer, device_id_type=MESH)

    scale[...] = jnp.broadcast_to(gain_ref[...], (PAD, rows)).T
    first = jax.nn.sigmoid(logits_ref[:, 0:1] - logits_ref[:, 1:2])
    second = jax.nn.sigmoid(logits_ref[:, 1:2] - logits_ref[:, 0:1])
    labels = lax.broadcasted_iota(jnp.int32, (count, PAD), 1)
    table = first * (experts_ref[:, 0:1] == labels).astype(jnp.float32)
    table = table + second * (experts_ref[:, 1:2] == labels).astype(jnp.float32)
    all_ref[f, :, :depth] = normalize(tokens_ref[...])
    all_ref[f, :, depth:] = table.astype(jnp.bfloat16)

    pl.semaphore_wait(barrier, fs_size + 1)

    def remote(a, b, send, recv, peer):
        return pltpu.make_async_remote_copy(
            src_ref=a, dst_ref=b, send_sem=send, recv_sem=recv, device_id=peer,
            device_id_type=MESH,
        )

    def row_copy(q, owner):
        return remote(
            all_ref.at[f], all_ref.at[owner], g_s.at[q], g_r.at[q], fs_peers[q]
        )

    def final(m, zs, xs, h):
        row = pl.multiple_of((zs * 2 + xs) * rows + h * chunk, chunk)
        return served.at[
            m, pl.ds(row, chunk), pl.ds(pl.multiple_of(c * width, width), width)
        ]

    def part_of(array, m, e, h):
        return array.at[m, e, pl.ds(pl.multiple_of(h * chunk, chunk), chunk)]

    def source_z(j):
        return jnp.where(j == 0, z, jnp.where(j == 1, near, jnp.where(j == 2, beyond, across)))

    def entry(k):
        r = k - group
        late = r - early - group
        mixed = r < early
        third, phase = lax.div(r, 3), lax.rem(r, 3)
        j = jnp.where(
            r < 0, 0,
            jnp.where(mixed, jnp.where(phase < 2, 1, 3), jnp.where(late < 0, 2, 3)),
        )
        g = jnp.where(
            r < 0, k,
            jnp.where(
                mixed, jnp.where(phase < 2, 2 * third + phase, third),
                jnp.where(late < 0, late + group, late + half),
            ),
        )
        return j, lax.div(g, PARTS), lax.rem(g, PARTS), source_z(j)

    def per_matrix(m, body):
        for n in range(matrices):
            pl.when(m == n)(functools.partial(body, n))

    def send_z(m, h, e):
        k = z * group + m * PARTS + h
        peer = (e * 2 + x, t)

        def go(here):
            remote(part_of(src, m, e, h), here, z_s.at[e * matrices + m], z_r.at[k], peer).start()

        pl.when(s == x)(lambda: go(final(m, z, x, h)))
        pl.when(s != x)(lambda: go(part_of(transit, m, z, h)))

    def send_c(m, j, zs, xs, h, q):
        here = final(m, zs, xs, h)
        n = (j * matrices + m) * 2 + q
        remote(here, here, c_s.at[n], c_r.at[n], c_peer).start()

    def run(home):
        def spread(m, j, zs, h, own):
            k = j * group + m * PARTS + h
            n = j * matrices + m
            if home:
                here = final(m, zs, x, h)
                remote(here, here, y_s.at[n], y_r.at[k], y_peer).start()
                send_c(m, j, zs, x, h, 0)
            else:
                here = part_of(src if own else transit, m, zs, h)
                remote(
                    here, part_of(transit, m, zs, h), y_s.at[n], y_r.at[k], y_peer
                ).start()
                remote(here, final(m, zs, x, h), x_s.at[n], x_r.at[k], x_peer).start()

        def round_group(m, g):
            h = lax.rem(g, PARTS)
            gain = scale[pl.ds(pl.multiple_of(h * chunk, chunk), chunk), 0:1]
            for e in range(experts):
                k = g * experts + e
                slot = lax.rem(k, SLOTS)
                pltpu.make_async_copy(
                    trained[m].at[e, pl.ds(0, chunk)], staged.at[slot], l_in.at[slot]
                ).wait()
                value = staged[slot]
                if m < 2:
                    value = gain * value
                value = value.astype(jnp.bfloat16)
                if home:
                    @pl.when(z == e)
                    def _():
                        final(m, z, x, h)[...] = value

                    @pl.when(z != e)
                    def _():
                        part_of(src, m, e, h)[...] = value
                else:
                    part_of(src, m, e, h)[...] = value

                @pl.when(k + SLOTS < total)
                def _():
                    load(k + SLOTS)

            spread(m, 0, z, h, True)
            send_z(m, h, near)

            @pl.when(jnp.logical_not(outer))
            def _():
                for e in far:
                    send_z(m, h, e)

        def gate_up(m, j, xs):
            zs = source_z(j)
            block = zs * 2 + xs
            q = jnp.where(xs == x, 0, 1)
            wait_c((j * matrices + m) * 2 + q)
            rows_in = rows_of(block)
            base = pl.multiple_of(block * rows, rows)

            @pl.loop(0, 2 * width // TILE)
            def _(i):
                col = pl.ds(pl.multiple_of(i * TILE, TILE), TILE)
                acts[m, :, col] += jnp.dot(
                    rows_in, served[m, pl.ds(base, rows), col],
                    preferred_element_type=jnp.float32,
                )

        def rows_of(block):
            col = pl.ds(pl.multiple_of(block * rows, rows), rows)
            picked = [all_ref[q, :, col].astype(jnp.float32) for q in range(fs_size)]
            return jnp.concatenate(picked, axis=0).astype(jnp.bfloat16)

        def wait_c(n):
            whole = whole_block()
            remote(whole, whole, c_s.at[n], c_r.at[n], c_peer).wait_recv()

        def whole_block():
            return served.at[0, pl.ds(0, rows), pl.ds(0, width)]

        def mix(j):
            zs = source_z(j)
            for xs in range(2):
                block = zs * 2 + xs
                q = jnp.where(xs == x, 0, 1)
                wait_c((j * matrices + 2) * 2 + q)
                base = pl.multiple_of(block * rows, rows)

                def add(n, value):
                    col = pl.ds(pl.multiple_of(n * TILE, TILE), TILE)
                    return value + lax.dot_general(
                        hidden_ref[:, col], served[2, pl.ds(base, rows), col],
                        (((1,), (1,)), ((), ())), preferred_element_type=jnp.float32,
                    )

                value = lax.fori_loop(
                    0, 2 * width // TILE, add, jnp.zeros((fs_size * count, rows), jnp.float32)
                )
                for q in range(fs_size):
                    part_ref[q, :, pl.ds(base, rows)] = value[q * count:(q + 1) * count]

        acts[...] = jnp.zeros_like(acts)
        rounds = group // PER_STEP
        behind = LAG_X + 2
        first = group + early
        ready = first + group + 2 * PARTS - half + behind
        duties = (
            (group + behind, 0, 0),
            (group + behind + 1, 1, 0),
            (first + behind, 0, 1),
            (first + behind + 1, 1, 1),
            (first + behind + 2, 0, 3),
            (first + PARTS + behind, 0, 2),
            (first + 2 * PARTS + behind, 1, 2),
            (ready, 1, 3),
        )

        @pl.loop(0, total + LAG_X)
        def _(i):
            @pl.when(i < rounds)
            def _():
                for u in range(PER_STEP):
                    g = i * PER_STEP + u
                    per_matrix(lax.div(g, PARTS), lambda m: round_group(m, g))

            @pl.when(i == 0)
            def _():
                for q in range(fs_size - 1):
                    row_copy(q, f).start()

            @pl.when((i >= LAG_Y) & (i < total + LAG_Y))
            def _():
                k = i - LAG_Y
                j, m, h, zs = entry(k)
                k = j * group + m * PARTS + h
                whole = part_of(transit, 0, 0, 0)
                remote(whole, whole, y_s.at[0], y_r.at[k], y_peer).wait_recv()

                def go(m):
                    if home:
                        remote(
                            part_of(transit, m, zs, h), final(m, zs, x, h),
                            x_s.at[j * matrices + m], x_r.at[k], x_peer,
                        ).start()
                    else:
                        send_c(m, j, zs, x, h, 0)

                go(m)

            @pl.when(i >= LAG_X)
            def _():
                k = i - LAG_X
                j, m, h, zs = entry(k)
                k = j * group + m * PARTS + h
                whole = part_of(transit, 0, 0, 0)
                remote(whole, whole, x_s.at[0], x_r.at[k], x_peer).wait_recv()
                send_c(m, j, zs, 1 - x, h, 1)

            @pl.when(outer & (i >= rounds) & (i < rounds + group))
            def _():
                g = i - rounds
                for e in far:
                    send_z(lax.div(g, PARTS), lax.rem(g, PARTS), e)

            @pl.when((i >= group) & (i < total))
            def _():
                j, m, h, zs = entry(i)
                whole = part_of(transit, 0, 0, 0)
                remote(
                    whole, whole, z_s.at[0], z_r.at[zs * group + m * PARTS + h], x_peer
                ).wait_recv()
                spread(m, j, zs, h, False)

            @pl.when(i == group)
            def _():
                for q in range(fs_size - 1):
                    row_copy(q, lax.rem(f + fs_size - q - 1, fs_size)).wait()

            active, m, j = False, 0, 0
            for step, matrix, unit in duties:
                active = active | (i == step)
                m = jnp.where(i == step, matrix, m)
                j = jnp.where(i == step, unit, j)

            @pl.when(active)
            def _():
                for xs in range(2):
                    gate_up(m, j, xs)

            @pl.when(i == ready + 1)
            def _():
                table = jnp.concatenate(
                    [all_ref[q, :, depth:].astype(jnp.float32) for q in range(fs_size)], axis=0
                )
                lane = lax.broadcasted_iota(jnp.int32, table.shape, 1)
                weight = jnp.sum(jnp.where(lane == z, table, 0.0), axis=1, keepdims=True)

                @pl.loop(0, 2 * width // TILE)
                def _(n):
                    col = pl.ds(pl.multiple_of(n * TILE, TILE), TILE)
                    gate_act, up_act = acts[0, :, col], acts[1, :, col]
                    hidden_ref[:, col] = (
                        weight * jax.nn.silu(gate_act) * up_act
                    ).astype(jnp.bfloat16)

            @pl.when((i > ready + 1) & (i < ready + 1 + experts))
            def _():
                mix(i - ready - 2)

        mix(experts - 1)
        block = whole_block()

        @pl.loop(0, experts * matrices)
        def _(n):
            remote(block, block, y_s.at[n], y_r.at[0], y_peer).wait_send()
            remote(block, block, x_s.at[n], x_r.at[0], x_peer).wait_send()
            for q in range(2):
                remote(block, block, c_s.at[2 * n + q], c_r.at[0], c_peer).wait_send()

            @pl.when(lax.div(n, matrices) != z)
            def _():
                remote(block, block, z_s.at[n], z_r.at[0], x_peer).wait_send()

    pl.when(s == x)(lambda: run(True))
    pl.when(s != x)(lambda: run(False))


def exchanged(tokens, route_experts, route_logits, norm_gain, gate_train, up_train, down_train, fs_size):
    experts, rows, width = gate_train.shape
    count, depth = tokens.shape
    matrices = 3
    total = matrices * PARTS * experts
    units = matrices * experts
    anywhere = pl.BlockSpec(memory_space=pl.ANY)
    in_vmem = pl.BlockSpec(memory_space=pltpu.VMEM)
    dma = pltpu.SemaphoreType.DMA
    return pl.pallas_call(
        exchange_kernel,
        in_specs=[in_vmem] * 4 + [anywhere] * 3,
        out_specs=[in_vmem, anywhere, in_vmem],
        out_shape=[
            pltpu.VMEM((matrices, fs_size * rows, 2 * width), jnp.bfloat16),
            jax.ShapeDtypeStruct((matrices, experts, rows, width), jnp.bfloat16),
            jax.ShapeDtypeStruct((fs_size, count, depth), jnp.float32),
        ],
        scratch_shapes=[
            pltpu.VMEM((matrices, experts, rows, width), jnp.bfloat16),
            pltpu.VMEM((SLOTS, rows // PARTS, width), jnp.float32),
            pltpu.VMEM((rows, PAD), jnp.float32),
            pltpu.VMEM((fs_size, count, depth + PAD), jnp.bfloat16),
            pltpu.VMEM((2, fs_size * count, 2 * width), jnp.float32),
            pltpu.VMEM((fs_size * count, 2 * width), jnp.bfloat16),
            dma((SLOTS,)),
            dma((units,)),
            dma((total,)),
            dma((units,)),
            dma((total,)),
            dma((units,)),
            dma((total,)),
            dma((2 * units,)),
            dma((2 * units,)),
            dma((fs_size - 1,)),
            dma((fs_size - 1,)),
        ],
        compiler_params=pltpu.CompilerParams(
            collective_id=0, has_side_effects=True, vmem_limit_bytes=VMEM_LIMIT
        ),
        name="exchange_weights",
    )(tokens, route_experts, route_logits, norm_gain[None, :], gate_train, up_train, down_train)


def reduce_kernel(part_ref, out_ref, landed, send, recv):
    f = lax.axis_index("fs")
    t = lax.axis_index("tp")
    fs_size = part_ref.shape[0]
    peers = [lax.rem(f + q, fs_size) for q in range(1, fs_size)]
    barrier = pltpu.get_barrier_semaphore()
    for peer in peers:
        pl.semaphore_signal(barrier, inc=1, device_id=(peer, t), device_id_type=MESH)
    pl.semaphore_wait(barrier, fs_size - 1)

    def copy(q, slot):
        return pltpu.make_async_remote_copy(
            src_ref=part_ref.at[peers[q]], dst_ref=landed.at[slot], send_sem=send.at[q],
            recv_sem=recv.at[q], device_id=(peers[q], t), device_id_type=MESH,
        )

    for q in range(fs_size - 1):
        copy(q, q).start()
    total = part_ref[f]
    for q in range(fs_size - 1):
        copy(q, q).wait()
        total = total + landed[q]
    out_ref[...] = total.astype(out_ref.dtype)


def reduced(part):
    fs_size, count, depth = part.shape
    in_vmem = pl.BlockSpec(memory_space=pltpu.VMEM)
    return pl.pallas_call(
        reduce_kernel,
        in_specs=[in_vmem],
        out_specs=in_vmem,
        out_shape=jax.ShapeDtypeStruct((count, depth), jnp.bfloat16),
        scratch_shapes=[
            pltpu.VMEM((fs_size - 1, count, depth), jnp.float32),
            pltpu.SemaphoreType.DMA((fs_size - 1,)),
            pltpu.SemaphoreType.DMA((fs_size - 1,)),
        ],
        compiler_params=pltpu.CompilerParams(
            collective_id=1, has_side_effects=True, vmem_limit_bytes=REDUCE_LIMIT
        ),
        name="reduce_rows",
    )(part)


def store_kernel(joined, gate_ref, up_ref, down_ref, sems):
    piece = joined.shape[1] // STORES
    copies = [
        pltpu.make_async_copy(
            joined.at[m, pl.ds(n * piece, piece)], out.at[0, pl.ds(n * piece, piece)],
            sems.at[m, n],
        )
        for m, out in enumerate((gate_ref, up_ref, down_ref))
        for n in range(STORES)
    ]
    for copy in copies:
        copy.start()
    for copy in copies:
        copy.wait()


def stored(joined):
    matrices, depth, width = joined.shape
    return pl.pallas_call(
        store_kernel,
        in_specs=[pl.BlockSpec(memory_space=pltpu.VMEM)],
        out_specs=[pl.BlockSpec(memory_space=pl.ANY)] * matrices,
        out_shape=[jax.ShapeDtypeStruct((1, depth, width), joined.dtype)] * matrices,
        scratch_shapes=[pltpu.SemaphoreType.DMA((matrices, STORES))],
        compiler_params=pltpu.CompilerParams(vmem_limit_bytes=REDUCE_LIMIT),
        name="store_weights",
    )(pltpu.with_memory_space_constraint(joined, pltpu.VMEM))


def per_device(tokens, route_experts, route_logits, norm_gain, gate_train, up_train, down_train):
    joined, _, partial = exchanged(
        tokens, route_experts, route_logits, norm_gain, gate_train, up_train, down_train,
        lax.axis_size("fs"),
    )
    return (*stored(joined), reduced(partial))


def two_by_two(fs_size, tp_size, experts):
    return fs_size == 2 * experts and tp_size == 4 and experts == 4


def choose(*args):
    fits = two_by_two(lax.axis_size("fs"), lax.axis_size("tp"), args[4].shape[0])
    return (per_device if fits else per_device_general)(*args)


def solution(mesh):
    return jax.shard_map(
        choose,
        mesh=mesh,
        in_specs=(
            P(("fs", "tp"), None),
            P(("fs", "tp"), None),
            P(("fs", "tp"), None),
            P("fs"),
            P(None, "fs", "tp"),
            P(None, "fs", "tp"),
            P(None, "fs", "tp"),
        ),
        out_specs=(
            P("fs", None, None),
            P("fs", None, None),
            P("fs", None, None),
            P(("fs", "tp"), None),
        ),
        check_vma=False,
    )
```

```python
import functools

import jax
import jax.numpy as jnp
from jax import lax
from jax.experimental import pallas as pl
from jax.experimental.pallas import tpu as pltpu
from jax.sharding import PartitionSpec as P

MESH = pl.DeviceIdType.MESH
PARTS = 8
LAG_Y = 2
LAG_X = 5
PER_STEP = 2
SLOTS = 4
TILE = 512
VMEM_LIMIT = 16400000
STORES = 4
STORE_LIMIT = 2000000
PAD = 128


def for_sending(array):
    return jax.tree.map(lambda a: a.astype(jnp.bfloat16) if a.dtype == jnp.float32 else a, array)


def normalize(tokens):
    values = tokens.astype(jnp.float32)
    row_mean = jnp.mean(values, axis=-1, keepdims=True)
    centered = values - row_mean
    row_var = jnp.mean(centered * centered, axis=-1, keepdims=True)
    return (centered * lax.rsqrt(row_var + 1e-05)).astype(jnp.bfloat16)


def per_device_general(tokens, route_experts, route_logits, norm_gain, gate_train, up_train, down_train):
    fs_size = lax.axis_size("fs")
    tp_size = lax.axis_size("tp")
    expert_count = gate_train.shape[0]
    slices = fs_size // expert_count
    scale = norm_gain[None, :, None]
    gate_half = (scale * gate_train).astype(jnp.bfloat16)
    up_half = (scale * up_train).astype(jnp.bfloat16)
    down_half = down_train.astype(jnp.bfloat16)
    swapped = (
        lax.all_to_all(gate_half, "tp", split_axis=1, concat_axis=2, tiled=True),
        lax.all_to_all(up_half, "tp", split_axis=1, concat_axis=2, tiled=True),
        lax.all_to_all(down_half, "tp", split_axis=1, concat_axis=2, tiled=True),
    )
    quarter = swapped[0].shape[1]
    hidden_total = swapped[0].shape[2]
    block_width = hidden_total // slices

    def split_quarter(matrix):
        blocks = matrix.reshape(expert_count, quarter, slices, block_width)
        return blocks.transpose(0, 2, 1, 3).reshape(expert_count * slices, quarter, block_width)

    owned = lax.all_to_all(
        for_sending(tuple((split_quarter(matrix) for matrix in swapped))),
        "fs",
        split_axis=0,
        concat_axis=1,
        tiled=True,
    )
    stacked = tuple((matrix.reshape(1, fs_size, 1, quarter, block_width) for matrix in owned))
    joined = jax.tree.map(
        lambda part, own: part.astype(own.dtype),
        lax.all_gather(for_sending(stacked), "tp", axis=2, tiled=True),
        stacked,
    )
    gate_serve, up_serve, down_serve = tuple(
        (matrix.reshape(1, fs_size * tp_size * quarter, block_width) for matrix in joined)
    )
    normed = normalize(tokens)
    first = jax.nn.sigmoid(route_logits[:, 0] - route_logits[:, 1])
    second = jax.nn.sigmoid(route_logits[:, 1] - route_logits[:, 0])
    labels = jnp.arange(expert_count, dtype=jnp.int32)
    table = first[:, None] * (route_experts[:, 0:1] == labels[None, :]).astype(jnp.float32)
    table = table + second[:, None] * (route_experts[:, 1:2] == labels[None, :]).astype(jnp.float32)
    table = table.astype(jnp.bfloat16)
    rows_all, table_all = (
        lax.all_gather(normed, "fs", axis=0, tiled=True),
        lax.all_gather(table, "fs", axis=0, tiled=True),
    )
    own_expert = lax.axis_index("fs") // slices
    selector = (labels == own_expert).astype(jnp.float32)
    weight = jnp.sum(table_all.astype(jnp.float32) * selector[None, :], axis=1)
    gate_act = jnp.dot(rows_all, gate_serve[0], preferred_element_type=jnp.float32)
    up_act = jnp.dot(rows_all, up_serve[0], preferred_element_type=jnp.float32)
    hidden = (weight[:, None] * jax.nn.silu(gate_act) * up_act).astype(jnp.bfloat16)
    down_own = down_serve[0]
    summed = lax.psum_scatter(
        lax.dot_general(
            hidden, down_own, (((1,), (1,)), ((), ())), preferred_element_type=jnp.float32
        ),
        "fs",
        scatter_dimension=0,
        tiled=True,
    )
    return (gate_serve, up_serve, down_serve, summed.astype(jnp.bfloat16))


def exchange_kernel(
    tokens_ref, experts_ref, logits_ref, gain_ref, gate_in, up_in, down_in,
    served, transit, mixed_ref,
    part_ref, landed, src, staged, scale, all_ref, acts, hidden_ref,
    l_in, z_s, z_r, y_s, y_r, x_s, x_r, c_s, c_r, g_s, g_r,
    p_s, p_r
):
    trained = (gate_in, up_in, down_in)
    matrices = len(trained)
    experts, rows, width = gate_in.shape
    fs_size, count, _ = all_ref.shape
    depth = tokens_ref.shape[1]
    chunk = rows // PARTS
    group = matrices * PARTS
    total = experts * group
    early = group * 5 // 12
    lead = group * 2 // 3
    f = lax.axis_index("fs")
    t = lax.axis_index("tp")
    z, x = lax.div(f, 2), lax.rem(f, 2)
    s, c = lax.div(t, 2), lax.rem(t, 2)
    y_peer = (f, (1 - s) * 2 + c)
    c_peer = (f, s * 2 + 1 - c)
    x_peer = (z * 2 + 1 - x, t)
    low = z < experts // 2
    outer = (z == 0) | (z == experts - 1)
    near = z + 1 - 2 * lax.rem(z, 2)
    across = jnp.where(low, experts // 2, experts // 2 - 1)
    beyond = jnp.where(low, experts - 1, 0)
    far = (jnp.where(c == 0, across, beyond), jnp.where(c == 0, beyond, across))

    def load(k):
        g, e = lax.div(k, experts), lax.rem(k, experts)
        slot = lax.rem(k, SLOTS)
        row = pl.multiple_of(lax.rem(g, PARTS) * chunk, chunk)
        for m in range(matrices):
            @pl.when(lax.div(g, PARTS) == m)
            def _():
                pltpu.make_async_copy(
                    trained[m].at[e, pl.ds(row, chunk)], staged.at[slot], l_in.at[slot]
                ).start()

    @pl.loop(0, SLOTS)
    def _(k):
        load(k)

    barrier = pltpu.get_barrier_semaphore()
    fs_peers = [(lax.rem(f + q, fs_size), t) for q in range(1, fs_size)]
    for peer in (*fs_peers, y_peer, c_peer):
        pl.semaphore_signal(barrier, inc=1, device_id=peer, device_id_type=MESH)

    scale[...] = jnp.broadcast_to(gain_ref[...], (PAD, rows)).T
    first = jax.nn.sigmoid(logits_ref[:, 0:1] - logits_ref[:, 1:2])
    second = jax.nn.sigmoid(logits_ref[:, 1:2] - logits_ref[:, 0:1])
    labels = lax.broadcasted_iota(jnp.int32, (count, PAD), 1)
    table = first * (experts_ref[:, 0:1] == labels).astype(jnp.float32)
    table = table + second * (experts_ref[:, 1:2] == labels).astype(jnp.float32)
    all_ref[f, :, :depth] = normalize(tokens_ref[...])
    all_ref[f, :, depth:] = table.astype(jnp.bfloat16)

    pl.semaphore_wait(barrier, fs_size + 1)

    def remote(a, b, send, recv, peer):
        return pltpu.make_async_remote_copy(
            src_ref=a, dst_ref=b, send_sem=send, recv_sem=recv, device_id=peer,
            device_id_type=MESH,
        )

    def row_copy(q, owner):
        return remote(
            all_ref.at[f], all_ref.at[owner], g_s.at[q], g_r.at[q], fs_peers[q]
        )

    def final(m, zs, xs, h):
        row = pl.multiple_of((zs * 2 + xs) * rows + h * chunk, chunk)
        return served.at[
            m, pl.ds(row, chunk), pl.ds(pl.multiple_of(c * width, width), width)
        ]

    def part_of(array, m, e, h):
        return array.at[m, e, pl.ds(pl.multiple_of(h * chunk, chunk), chunk)]

    def source_z(j):
        return jnp.where(j == 0, z, jnp.where(j == 1, near, jnp.where(j == 2, beyond, across)))

    def entry(k):
        r = k - group
        third, phase = lax.div(r, 3), lax.rem(r, 3)
        q = r - group - early
        pair = q - lead
        tail = pair - 2 * (group - lead)
        step = lax.div(pair, 2)
        even = lax.rem(pair, 2) == 0
        spans = (
            (r < 0, 0, k),
            ((r < 3 * early) & (phase < 2), 1, 2 * third + phase),
            (r < 3 * early, 3, third),
            (q < 0, 1, r - early),
            (pair < 0, 2, q),
            ((tail < 0) & even, 2, lead + step),
            (tail < 0, 3, early + step),
        )
        j, g = 3, early + group - lead + tail
        for test, unit, index in reversed(spans):
            j, g = jnp.where(test, unit, j), jnp.where(test, index, g)
        return j, lax.div(g, PARTS), lax.rem(g, PARTS), source_z(j)

    def per_matrix(m, body):
        for n in range(matrices):
            pl.when(m == n)(functools.partial(body, n))

    def send_z(m, h, e):
        k = z * group + m * PARTS + h
        peer = (e * 2 + x, t)

        def go(here):
            remote(part_of(src, m, e, h), here, z_s.at[e * matrices + m], z_r.at[k], peer).start()

        pl.when(s == x)(lambda: go(final(m, z, x, h)))
        pl.when(s != x)(lambda: go(part_of(transit, m, z, h)))

    def send_c(m, j, zs, xs, h, q):
        here = final(m, zs, xs, h)
        n = (j * matrices + m) * 2 + q
        remote(here, here, c_s.at[n], c_r.at[n], c_peer).start()

    def run(home):
        def spread(m, j, zs, h, own):
            k = j * group + m * PARTS + h
            n = j * matrices + m
            if home:
                here = final(m, zs, x, h)
                remote(here, here, y_s.at[n], y_r.at[k], y_peer).start()
                send_c(m, j, zs, x, h, 0)
            else:
                here = part_of(src if own else transit, m, zs, h)
                remote(
                    here, part_of(transit, m, zs, h), y_s.at[n], y_r.at[k], y_peer
                ).start()
                remote(here, final(m, zs, x, h), x_s.at[n], x_r.at[k], x_peer).start()

        def round_group(m, g):
            h = lax.rem(g, PARTS)
            gain = scale[pl.ds(pl.multiple_of(h * chunk, chunk), chunk), 0:1]
            for e in range(experts):
                k = g * experts + e
                slot = lax.rem(k, SLOTS)
                pltpu.make_async_copy(
                    trained[m].at[e, pl.ds(0, chunk)], staged.at[slot], l_in.at[slot]
                ).wait()
                value = staged[slot]
                if m < 2:
                    value = gain * value
                value = value.astype(jnp.bfloat16)
                if home:
                    @pl.when(z == e)
                    def _():
                        final(m, z, x, h)[...] = value

                    @pl.when(z != e)
                    def _():
                        part_of(src, m, e, h)[...] = value
                else:
                    part_of(src, m, e, h)[...] = value

                @pl.when(k + SLOTS < total)
                def _():
                    load(k + SLOTS)

            spread(m, 0, z, h, True)
            send_z(m, h, near)

            @pl.when(jnp.logical_not(outer))
            def _():
                for e in far:
                    send_z(m, h, e)

        def gate_up(m, j):
            zs = source_z(j)
            for q in range(2):
                wait_c((j * matrices + m) * 2 + q)
            base = pl.ds(pl.multiple_of(zs * 2 * rows, 2 * rows), 2 * rows)
            picked = [all_ref[q, :, base].astype(jnp.float32) for q in range(fs_size)]
            rows_in = jnp.concatenate(picked, axis=0).astype(jnp.bfloat16)

            @pl.loop(0, 2 * width // TILE)
            def _(i):
                col = pl.ds(pl.multiple_of(i * TILE, TILE), TILE)
                acts[m, :, col] += jnp.dot(
                    rows_in, served[m, base, col], preferred_element_type=jnp.float32
                )

        def wait_c(n):
            whole = whole_block()
            remote(whole, whole, c_s.at[n], c_r.at[n], c_peer).wait_recv()

        def whole_block():
            return served.at[0, pl.ds(0, rows), pl.ds(0, width)]

        def mix(j):
            for q in range(2):
                wait_c((j * matrices + 2) * 2 + q)
            base = pl.ds(pl.multiple_of(source_z(j) * 2 * rows, 2 * rows), 2 * rows)

            def add(n, value):
                col = pl.ds(pl.multiple_of(n * TILE, TILE), TILE)
                return value + lax.dot_general(
                    hidden_ref[:, col], served[2, base, col],
                    (((1,), (1,)), ((), ())), preferred_element_type=jnp.float32,
                )

            value = lax.fori_loop(
                0, 2 * width // TILE, add, jnp.zeros((fs_size * count, 2 * rows), jnp.float32)
            )
            for q in range(fs_size):
                part_ref[q, :, base] = value[q * count:(q + 1) * count]

        acts[...] = jnp.zeros_like(acts)
        rounds = group // PER_STEP
        behind = LAG_X + 2
        first = 2 * group + early
        ready = first + lead + 2 * (2 * PARTS - early) + behind
        duties = (
            (group + behind, 0, 0),
            (group + behind + 1, 1, 0),
            (first + behind, 0, 1),
            (first + behind + 1, 1, 1),
            (first + behind + 2, 0, 3),
            (first + PARTS + behind, 0, 2),
            (first + 2 * PARTS + behind, 1, 2),
            (ready, 1, 3),
        )

        @pl.loop(0, total + LAG_X)
        def _(i):
            @pl.when(i < rounds)
            def _():
                for u in range(PER_STEP):
                    g = i * PER_STEP + u
                    per_matrix(lax.div(g, PARTS), lambda m: round_group(m, g))

            @pl.when(i == 0)
            def _():
                for q in range(fs_size - 1):
                    row_copy(q, f).start()

            @pl.when((i >= LAG_Y) & (i < total + LAG_Y))
            def _():
                k = i - LAG_Y
                j, m, h, zs = entry(k)
                k = j * group + m * PARTS + h
                whole = part_of(transit, 0, 0, 0)
                remote(whole, whole, y_s.at[0], y_r.at[k], y_peer).wait_recv()

                def go(m):
                    if home:
                        remote(
                            part_of(transit, m, zs, h), final(m, zs, x, h),
                            x_s.at[j * matrices + m], x_r.at[k], x_peer,
                        ).start()
                    else:
                        send_c(m, j, zs, x, h, 0)

                go(m)

            @pl.when(i >= LAG_X)
            def _():
                k = i - LAG_X
                j, m, h, zs = entry(k)
                k = j * group + m * PARTS + h
                whole = part_of(transit, 0, 0, 0)
                remote(whole, whole, x_s.at[0], x_r.at[k], x_peer).wait_recv()
                send_c(m, j, zs, 1 - x, h, 1)

            @pl.when(outer & (i >= rounds) & (i < rounds + group))
            def _():
                g = i - rounds
                for e in far:
                    send_z(lax.div(g, PARTS), lax.rem(g, PARTS), e)

            @pl.when((i >= group) & (i < total))
            def _():
                j, m, h, zs = entry(i)
                whole = part_of(transit, 0, 0, 0)
                remote(
                    whole, whole, z_s.at[0], z_r.at[zs * group + m * PARTS + h], x_peer
                ).wait_recv()
                spread(m, j, zs, h, False)

            @pl.when(i == group)
            def _():
                for q in range(fs_size - 1):
                    row_copy(q, lax.rem(f + fs_size - q - 1, fs_size)).wait()

            active, m, j = False, 0, 0
            for step, matrix, unit in duties:
                active = active | (i == step)
                m = jnp.where(i == step, matrix, m)
                j = jnp.where(i == step, unit, j)

            @pl.when(active)
            def _():
                gate_up(m, j)

            @pl.when(i == ready + 1)
            def _():
                table = jnp.concatenate(
                    [all_ref[q, :, depth:].astype(jnp.float32) for q in range(fs_size)], axis=0
                )
                lane = lax.broadcasted_iota(jnp.int32, table.shape, 1)
                weight = jnp.sum(jnp.where(lane == z, table, 0.0), axis=1, keepdims=True)

                @pl.loop(0, 2 * width // TILE)
                def _(n):
                    col = pl.ds(pl.multiple_of(n * TILE, TILE), TILE)
                    gate_act, up_act = acts[0, :, col], acts[1, :, col]
                    hidden_ref[:, col] = (
                        weight * jax.nn.silu(gate_act) * up_act
                    ).astype(jnp.bfloat16)

            @pl.when((i > ready + 1) & (i < ready + 1 + experts))
            def _():
                mix(i - ready - 2)

        mix(experts - 1)

        def part_copy(q):
            to = lax.rem(f + q + 1, fs_size)
            return remote(part_ref.at[to], landed.at[q], p_s.at[q], p_r.at[q], fs_peers[q])

        for q in range(fs_size - 1):
            part_copy(q).start()
        block = whole_block()

        @pl.loop(0, experts * matrices)
        def _(n):
            remote(block, block, y_s.at[n], y_r.at[0], y_peer).wait_send()
            remote(block, block, x_s.at[n], x_r.at[0], x_peer).wait_send()
            for q in range(2):
                remote(block, block, c_s.at[2 * n + q], c_r.at[0], c_peer).wait_send()

            @pl.when(lax.div(n, matrices) != z)
            def _():
                remote(block, block, z_s.at[n], z_r.at[0], x_peer).wait_send()

        summed = part_ref[f]
        for q in range(fs_size - 1):
            part_copy(q).wait()
            summed = summed + landed[q]
        mixed_ref[...] = summed.astype(mixed_ref.dtype)

    pl.when(s == x)(lambda: run(True))
    pl.when(s != x)(lambda: run(False))


def exchanged(tokens, route_experts, route_logits, norm_gain, gate_train, up_train, down_train, fs_size):
    experts, rows, width = gate_train.shape
    count, depth = tokens.shape
    matrices = 3
    total = matrices * PARTS * experts
    units = matrices * experts
    anywhere = pl.BlockSpec(memory_space=pl.ANY)
    in_vmem = pl.BlockSpec(memory_space=pltpu.VMEM)
    dma = pltpu.SemaphoreType.DMA
    return pl.pallas_call(
        exchange_kernel,
        in_specs=[in_vmem] * 4 + [anywhere] * 3,
        out_specs=[in_vmem, anywhere, in_vmem],
        out_shape=[
            pltpu.VMEM((matrices, fs_size * rows, 2 * width), jnp.bfloat16),
            jax.ShapeDtypeStruct((matrices, experts, rows, width), jnp.bfloat16),
            jax.ShapeDtypeStruct((count, depth), jnp.bfloat16),
        ],
        scratch_shapes=[
            pltpu.VMEM((fs_size, count, depth), jnp.float32),
            pltpu.VMEM((fs_size - 1, count, depth), jnp.float32),
            pltpu.VMEM((matrices, experts, rows, width), jnp.bfloat16),
            pltpu.VMEM((SLOTS, rows // PARTS, width), jnp.float32),
            pltpu.VMEM((rows, PAD), jnp.float32),
            pltpu.VMEM((fs_size, count, depth + PAD), jnp.bfloat16),
            pltpu.VMEM((2, fs_size * count, 2 * width), jnp.float32),
            pltpu.VMEM((fs_size * count, 2 * width), jnp.bfloat16),
            dma((SLOTS,)),
            dma((units,)),
            dma((total,)),
            dma((units,)),
            dma((total,)),
            dma((units,)),
            dma((total,)),
            dma((2 * units,)),
            dma((2 * units,)),
            dma((fs_size - 1,)),
            dma((fs_size - 1,)),
            dma((fs_size - 1,)),
            dma((fs_size - 1,)),
        ],
        compiler_params=pltpu.CompilerParams(
            collective_id=0, has_side_effects=True, vmem_limit_bytes=VMEM_LIMIT
        ),
        name="exchange_weights",
    )(tokens, route_experts, route_logits, norm_gain[None, :], gate_train, up_train, down_train)


def store_kernel(joined, gate_ref, up_ref, down_ref, sems):
    piece = joined.shape[1] // STORES
    copies = [
        pltpu.make_async_copy(
            joined.at[m, pl.ds(n * piece, piece)], out.at[0, pl.ds(n * piece, piece)],
            sems.at[m, n],
        )
        for m, out in enumerate((gate_ref, up_ref, down_ref))
        for n in range(STORES)
    ]
    for copy in copies:
        copy.start()
    for copy in copies:
        copy.wait()


def stored(joined):
    matrices, depth, width = joined.shape
    return pl.pallas_call(
        store_kernel,
        in_specs=[pl.BlockSpec(memory_space=pltpu.VMEM)],
        out_specs=[pl.BlockSpec(memory_space=pl.ANY)] * matrices,
        out_shape=[jax.ShapeDtypeStruct((1, depth, width), joined.dtype)] * matrices,
        scratch_shapes=[pltpu.SemaphoreType.DMA((matrices, STORES))],
        compiler_params=pltpu.CompilerParams(vmem_limit_bytes=STORE_LIMIT),
        name="store_weights",
    )(pltpu.with_memory_space_constraint(joined, pltpu.VMEM))


def per_device(tokens, route_experts, route_logits, norm_gain, gate_train, up_train, down_train):
    joined, _, mixed = exchanged(
        tokens, route_experts, route_logits, norm_gain, gate_train, up_train, down_train,
        lax.axis_size("fs"),
    )
    return (*stored(joined), mixed)


def two_by_two(fs_size, tp_size, experts):
    return fs_size == 2 * experts and tp_size == 4 and experts == 4


def choose(*args):
    fits = two_by_two(lax.axis_size("fs"), lax.axis_size("tp"), args[4].shape[0])
    return (per_device if fits else per_device_general)(*args)


def solution(mesh):
    return jax.shard_map(
        choose,
        mesh=mesh,
        in_specs=(
            P(("fs", "tp"), None),
            P(("fs", "tp"), None),
            P(("fs", "tp"), None),
            P("fs"),
            P(None, "fs", "tp"),
            P(None, "fs", "tp"),
            P(None, "fs", "tp"),
        ),
        out_specs=(
            P("fs", None, None),
            P("fs", None, None),
            P("fs", None, None),
            P(("fs", "tp"), None),
        ),
        check_vma=False,
    )
```

```python
import functools

import jax
import jax.numpy as jnp
from jax import lax
from jax.experimental import pallas as pl
from jax.experimental.pallas import tpu as pltpu
from jax.sharding import PartitionSpec as P

MESH = pl.DeviceIdType.MESH
PARTS = 8
LAG_Y = 2
LAG_X = 5
PER_STEP = 1
SLOTS = 4
TILE = 1024
SUB = 4
VMEM_LIMIT = 16400000
STORES = 4
STORE_LIMIT = 2000000
PAD = 128


def for_sending(array):
    return jax.tree.map(lambda a: a.astype(jnp.bfloat16) if a.dtype == jnp.float32 else a, array)


def normalize(tokens):
    values = tokens.astype(jnp.float32)
    row_mean = jnp.mean(values, axis=-1, keepdims=True)
    centered = values - row_mean
    row_var = jnp.mean(centered * centered, axis=-1, keepdims=True)
    return (centered * lax.rsqrt(row_var + 1e-05)).astype(jnp.bfloat16)


def per_device_general(tokens, route_experts, route_logits, norm_gain, gate_train, up_train, down_train):
    fs_size = lax.axis_size("fs")
    tp_size = lax.axis_size("tp")
    expert_count = gate_train.shape[0]
    slices = fs_size // expert_count
    scale = norm_gain[None, :, None]
    gate_half = (scale * gate_train).astype(jnp.bfloat16)
    up_half = (scale * up_train).astype(jnp.bfloat16)
    down_half = down_train.astype(jnp.bfloat16)
    swapped = (
        lax.all_to_all(gate_half, "tp", split_axis=1, concat_axis=2, tiled=True),
        lax.all_to_all(up_half, "tp", split_axis=1, concat_axis=2, tiled=True),
        lax.all_to_all(down_half, "tp", split_axis=1, concat_axis=2, tiled=True),
    )
    quarter = swapped[0].shape[1]
    hidden_total = swapped[0].shape[2]
    block_width = hidden_total // slices

    def split_quarter(matrix):
        blocks = matrix.reshape(expert_count, quarter, slices, block_width)
        return blocks.transpose(0, 2, 1, 3).reshape(expert_count * slices, quarter, block_width)

    owned = lax.all_to_all(
        for_sending(tuple((split_quarter(matrix) for matrix in swapped))),
        "fs",
        split_axis=0,
        concat_axis=1,
        tiled=True,
    )
    stacked = tuple((matrix.reshape(1, fs_size, 1, quarter, block_width) for matrix in owned))
    joined = jax.tree.map(
        lambda part, own: part.astype(own.dtype),
        lax.all_gather(for_sending(stacked), "tp", axis=2, tiled=True),
        stacked,
    )
    gate_serve, up_serve, down_serve = tuple(
        (matrix.reshape(1, fs_size * tp_size * quarter, block_width) for matrix in joined)
    )
    normed = normalize(tokens)
    first = jax.nn.sigmoid(route_logits[:, 0] - route_logits[:, 1])
    second = jax.nn.sigmoid(route_logits[:, 1] - route_logits[:, 0])
    labels = jnp.arange(expert_count, dtype=jnp.int32)
    table = first[:, None] * (route_experts[:, 0:1] == labels[None, :]).astype(jnp.float32)
    table = table + second[:, None] * (route_experts[:, 1:2] == labels[None, :]).astype(jnp.float32)
    table = table.astype(jnp.bfloat16)
    rows_all, table_all = (
        lax.all_gather(normed, "fs", axis=0, tiled=True),
        lax.all_gather(table, "fs", axis=0, tiled=True),
    )
    own_expert = lax.axis_index("fs") // slices
    selector = (labels == own_expert).astype(jnp.float32)
    weight = jnp.sum(table_all.astype(jnp.float32) * selector[None, :], axis=1)
    gate_act = jnp.dot(rows_all, gate_serve[0], preferred_element_type=jnp.float32)
    up_act = jnp.dot(rows_all, up_serve[0], preferred_element_type=jnp.float32)
    hidden = (weight[:, None] * jax.nn.silu(gate_act) * up_act).astype(jnp.bfloat16)
    down_own = down_serve[0]
    summed = lax.psum_scatter(
        lax.dot_general(
            hidden, down_own, (((1,), (1,)), ((), ())), preferred_element_type=jnp.float32
        ),
        "fs",
        scatter_dimension=0,
        tiled=True,
    )
    return (gate_serve, up_serve, down_serve, summed.astype(jnp.bfloat16))


def exchange_kernel(
    tokens_ref, experts_ref, logits_ref, gain_ref, gate_in, up_in, down_in,
    served, transit, mixed_ref,
    part_ref, landed, src, staged, scale, all_ref, acts, hidden_ref,
    l_in, z_s, z_r, y_s, y_r, x_s, x_r, c_s, c_r, g_s, g_r,
    p_s, p_r, zt_r, yt_r, xt_r
):
    trained = (gate_in, up_in, down_in)
    matrices = len(trained)
    experts, rows, width = gate_in.shape
    fs_size, count, _ = all_ref.shape
    depth = tokens_ref.shape[1]
    chunk = rows // PARTS
    group = matrices * PARTS
    total = experts * group
    early = group * 5 // 12
    lead = group * 2 // 3
    f = lax.axis_index("fs")
    t = lax.axis_index("tp")
    z, x = lax.div(f, 2), lax.rem(f, 2)
    s, c = lax.div(t, 2), lax.rem(t, 2)
    y_peer = (f, (1 - s) * 2 + c)
    c_peer = (f, s * 2 + 1 - c)
    x_peer = (z * 2 + 1 - x, t)
    low = z < experts // 2
    outer = (z == 0) | (z == experts - 1)
    near = z + 1 - 2 * lax.rem(z, 2)
    across = jnp.where(low, experts // 2, experts // 2 - 1)
    beyond = jnp.where(low, experts - 1, 0)
    far = (jnp.where(c == 0, across, beyond), jnp.where(c == 0, beyond, across))

    def load(k):
        g, e = lax.div(k, experts), lax.rem(k, experts)
        slot = lax.rem(k, SLOTS)
        row = pl.multiple_of(lax.rem(g, PARTS) * chunk, chunk)
        for m in range(matrices):
            @pl.when(lax.div(g, PARTS) == m)
            def _():
                pltpu.make_async_copy(
                    trained[m].at[e, pl.ds(row, chunk)], staged.at[slot], l_in.at[slot]
                ).start()

    @pl.loop(0, SLOTS)
    def _(k):
        load(k)

    barrier = pltpu.get_barrier_semaphore()
    fs_peers = [(lax.rem(f + q, fs_size), t) for q in range(1, fs_size)]
    for peer in (*fs_peers, y_peer, c_peer):
        pl.semaphore_signal(barrier, inc=1, device_id=peer, device_id_type=MESH)

    scale[...] = jnp.broadcast_to(gain_ref[...], (PAD, rows)).T
    first = jax.nn.sigmoid(logits_ref[:, 0:1] - logits_ref[:, 1:2])
    second = jax.nn.sigmoid(logits_ref[:, 1:2] - logits_ref[:, 0:1])
    labels = lax.broadcasted_iota(jnp.int32, (count, PAD), 1)
    table = first * (experts_ref[:, 0:1] == labels).astype(jnp.float32)
    table = table + second * (experts_ref[:, 1:2] == labels).astype(jnp.float32)
    all_ref[f, :, :depth] = normalize(tokens_ref[...])
    all_ref[f, :, depth:] = table.astype(jnp.bfloat16)

    pl.semaphore_wait(barrier, fs_size + 1)

    def remote(a, b, send, recv, peer):
        return pltpu.make_async_remote_copy(
            src_ref=a, dst_ref=b, send_sem=send, recv_sem=recv, device_id=peer,
            device_id_type=MESH,
        )

    def row_copy(q, owner):
        return remote(
            all_ref.at[f], all_ref.at[owner], g_s.at[q], g_r.at[q], fs_peers[q]
        )

    def span(start, u):
        size = chunk if u is None else chunk // SUB
        return pl.ds(pl.multiple_of(start + (0 if u is None else u * size), size), size)

    def final(m, zs, xs, h, u=None):
        return served.at[
            m, span((zs * 2 + xs) * rows + h * chunk, u),
            pl.ds(pl.multiple_of(c * width, width), width),
        ]

    def part_of(array, m, e, h, u=None):
        return array.at[m, e, span(h * chunk, u)]

    def source_z(j):
        return jnp.where(j == 0, z, jnp.where(j == 1, near, jnp.where(j == 2, beyond, across)))

    def entry(k):
        r = k - group
        third, phase = lax.div(r, 3), lax.rem(r, 3)
        q = r - group - early
        pair = q - lead
        tail = pair - 2 * (group - lead)
        step = lax.div(pair, 2)
        even = lax.rem(pair, 2) == 0
        spans = (
            (r < 0, 0, k),
            ((r < 3 * early) & (phase < 2), 1, 2 * third + phase),
            (r < 3 * early, 3, third),
            (q < 0, 1, r - early),
            (pair < 0, 2, q),
            ((tail < 0) & even, 2, lead + step),
            (tail < 0, 3, early + step),
        )
        j, g = 3, early + group - lead + tail
        for test, unit, index in reversed(spans):
            j, g = jnp.where(test, unit, j), jnp.where(test, index, g)
        return j, lax.div(g, PARTS), lax.rem(g, PARTS), source_z(j)

    def per_matrix(m, body):
        for n in range(matrices):
            pl.when(m == n)(functools.partial(body, n))

    def send_z(m, h, e, u=None):
        k = z * group + m * PARTS + h
        recv = z_r.at[k] if u is None else zt_r.at[u]
        peer = (e * 2 + x, t)

        def go(there):
            remote(part_of(src, m, e, h, u), there, z_s.at[e * matrices + m], recv, peer).start()

        pl.when(s == x)(lambda: go(final(m, z, x, h, u)))
        pl.when(s != x)(lambda: go(part_of(transit, m, z, h, u)))

    def send_c(m, j, zs, xs, h, q, u=None):
        here = final(m, zs, xs, h, u)
        n = (j * matrices + m) * 2 + q
        remote(here, here, c_s.at[n], c_r.at[n], c_peer).start()

    def run(home):
        def spread(m, j, zs, h, own, u=None):
            k = j * group + m * PARTS + h
            n = j * matrices + m
            y_recv, x_recv = (y_r.at[k], x_r.at[k]) if u is None else (yt_r.at[u], xt_r.at[u])
            if home:
                here = final(m, zs, x, h, u)
                remote(here, here, y_s.at[n], y_recv, y_peer).start()
                send_c(m, j, zs, x, h, 0, u)
            else:
                here = part_of(src if own else transit, m, zs, h, u)
                remote(
                    here, part_of(transit, m, zs, h, u), y_s.at[n], y_recv, y_peer
                ).start()
                remote(here, final(m, zs, x, h, u), x_s.at[n], x_recv, x_peer).start()

        def from_z(k, u=None):
            j, m, h, zs = entry(k)
            whole = part_of(transit, 0, 0, 0, u)
            recv = z_r.at[zs * group + m * PARTS + h] if u is None else zt_r.at[u]
            remote(whole, whole, z_s.at[0], recv, x_peer).wait_recv()
            spread(m, j, zs, h, False, u)

        def from_y(k, u=None):
            j, m, h, zs = entry(k)
            n = j * group + m * PARTS + h
            whole = part_of(transit, 0, 0, 0, u)
            recv = y_r.at[n] if u is None else yt_r.at[u]
            remote(whole, whole, y_s.at[0], recv, y_peer).wait_recv()
            if home:
                recv = x_r.at[n] if u is None else xt_r.at[u]
                remote(
                    part_of(transit, m, zs, h, u), final(m, zs, x, h, u),
                    x_s.at[j * matrices + m], recv, x_peer,
                ).start()
            else:
                send_c(m, j, zs, x, h, 0, u)

        def from_x(k, u=None):
            j, m, h, zs = entry(k)
            n = j * group + m * PARTS + h
            whole = part_of(transit, 0, 0, 0, u)
            recv = x_r.at[n] if u is None else xt_r.at[u]
            remote(whole, whole, x_s.at[0], recv, x_peer).wait_recv()
            send_c(m, j, zs, 1 - x, h, 1, u)

        def round_group(m, g):
            h = lax.rem(g, PARTS)
            gain = scale[pl.ds(pl.multiple_of(h * chunk, chunk), chunk), 0:1]
            for e in range(experts):
                k = g * experts + e
                slot = lax.rem(k, SLOTS)
                pltpu.make_async_copy(
                    trained[m].at[e, pl.ds(0, chunk)], staged.at[slot], l_in.at[slot]
                ).wait()
                value = staged[slot]
                if m < 2:
                    value = gain * value
                value = value.astype(jnp.bfloat16)
                if home:
                    @pl.when(z == e)
                    def _():
                        final(m, z, x, h)[...] = value

                    @pl.when(z != e)
                    def _():
                        part_of(src, m, e, h)[...] = value
                else:
                    part_of(src, m, e, h)[...] = value

                @pl.when(k + SLOTS < total)
                def _():
                    load(k + SLOTS)

            spread(m, 0, z, h, True)
            send_z(m, h, near)

            @pl.when(jnp.logical_not(outer))
            def _():
                if m < matrices - 1:
                    for e in far:
                        send_z(m, h, e)
                else:
                    @pl.when(h < PARTS - 1)
                    def _():
                        for e in far:
                            send_z(m, h, e)

                    @pl.when(h == PARTS - 1)
                    def _():
                        for e in far:
                            for u in range(SUB):
                                send_z(m, h, e, u)

        def gate_up(m, j):
            zs = source_z(j)
            for q in range(2):
                wait_c((j * matrices + m) * 2 + q)
            base = pl.ds(pl.multiple_of(zs * 2 * rows, 2 * rows), 2 * rows)
            picked = [all_ref[q, :, base].astype(jnp.float32) for q in range(fs_size)]
            rows_in = jnp.concatenate(picked, axis=0).astype(jnp.bfloat16)

            @pl.loop(0, 2 * width // TILE)
            def _(i):
                col = pl.ds(pl.multiple_of(i * TILE, TILE), TILE)
                acts[m, :, col] += jnp.dot(
                    rows_in, served[m, base, col], preferred_element_type=jnp.float32
                )

        def wait_c(n):
            whole = whole_block()
            remote(whole, whole, c_s.at[n], c_r.at[n], c_peer).wait_recv()

        def whole_block():
            return served.at[0, pl.ds(0, rows), pl.ds(0, width)]

        def mix(j):
            for q in range(2):
                wait_c((j * matrices + 2) * 2 + q)
            base = pl.ds(pl.multiple_of(source_z(j) * 2 * rows, 2 * rows), 2 * rows)

            def add(n, value):
                col = pl.ds(pl.multiple_of(n * TILE, TILE), TILE)
                return value + lax.dot_general(
                    hidden_ref[:, col], served[2, base, col],
                    (((1,), (1,)), ((), ())), preferred_element_type=jnp.float32,
                )

            value = lax.fori_loop(
                0, 2 * width // TILE, add, jnp.zeros((fs_size * count, 2 * rows), jnp.float32)
            )
            for q in range(fs_size):
                part_ref[q, :, base] = value[q * count:(q + 1) * count]

        acts[...] = jnp.zeros_like(acts)
        rounds = group // PER_STEP
        behind = LAG_X + 1
        first = 2 * group + early
        ready = first + lead + 2 * (2 * PARTS - early) + behind
        duties = (
            (group + behind, 0, 0),
            (group + behind + 1, 1, 0),
            (first + behind, 0, 1),
            (first + behind + 1, 1, 1),
            (first + behind + 2, 0, 3),
            (first + PARTS + behind, 0, 2),
            (first + 2 * PARTS + behind, 1, 2),
            (ready, 1, 3),
        )

        @pl.loop(0, total - 1)
        def _(i):
            pl.when(i >= LAG_Y)(lambda: from_y(i - LAG_Y))
            pl.when(i >= LAG_X)(lambda: from_x(i - LAG_X))

            @pl.when(i < rounds)
            def _():
                for u in range(PER_STEP):
                    g = i * PER_STEP + u
                    per_matrix(lax.div(g, PARTS), lambda m: round_group(m, g))

            @pl.when(i == 0)
            def _():
                for q in range(fs_size - 1):
                    row_copy(q, f).start()

            @pl.when(outer & (i >= rounds) & (i < rounds + group))
            def _():
                g = i - rounds
                for e in far:
                    send_z(lax.div(g, PARTS), lax.rem(g, PARTS), e)

            pl.when(i >= group)(lambda: from_z(i))

            @pl.when(i == group)
            def _():
                for q in range(fs_size - 1):
                    row_copy(q, lax.rem(f + fs_size - q - 1, fs_size)).wait()

            active, m, j = False, 0, 0
            for step, matrix, unit in duties:
                active = active | (i == step)
                m = jnp.where(i == step, matrix, m)
                j = jnp.where(i == step, unit, j)

            @pl.when(active)
            def _():
                gate_up(m, j)

            @pl.when(i == ready + 1)
            def _():
                table = jnp.concatenate(
                    [all_ref[q, :, depth:].astype(jnp.float32) for q in range(fs_size)], axis=0
                )
                lane = lax.broadcasted_iota(jnp.int32, table.shape, 1)
                weight = jnp.sum(jnp.where(lane == z, table, 0.0), axis=1, keepdims=True)

                @pl.loop(0, 2 * width // TILE)
                def _(n):
                    col = pl.ds(pl.multiple_of(n * TILE, TILE), TILE)
                    gate_act, up_act = acts[0, :, col], acts[1, :, col]
                    hidden_ref[:, col] = (
                        weight * jax.nn.silu(gate_act) * up_act
                    ).astype(jnp.bfloat16)

            @pl.when(i == ready + 2)
            def _():
                mix(0)

        last = total - 1
        for k in range(last - LAG_Y, last - 1):
            from_y(k)
        for k in range(last - LAG_X, last - 2):
            from_x(k)
        tail = [(from_z, last, u) for u in range(SUB)]
        tail[SUB // 2:SUB // 2] = [(from_y, last - 1, None), (from_x, last - 2, None)]
        tail.append((from_x, last - 1, None))
        for u in range(SUB):
            tail.append((from_y, last, u))
            if u:
                tail.append((from_x, last, u - 1))
        tail.append((from_x, last, SUB - 1))
        for n, (step, k, u) in enumerate(tail):
            if n == SUB + 2:
                mix(1)
            if n == SUB + 5:
                mix(2)
            step(k, u)
        mix(experts - 1)

        def part_copy(q):
            to = lax.rem(f + q + 1, fs_size)
            return remote(part_ref.at[to], landed.at[q], p_s.at[q], p_r.at[q], fs_peers[q])

        for q in range(fs_size - 1):
            part_copy(q).start()
        block = whole_block()

        @pl.loop(0, experts * matrices)
        def _(n):
            remote(block, block, y_s.at[n], y_r.at[0], y_peer).wait_send()
            remote(block, block, x_s.at[n], x_r.at[0], x_peer).wait_send()
            for q in range(2):
                remote(block, block, c_s.at[2 * n + q], c_r.at[0], c_peer).wait_send()

            @pl.when(lax.div(n, matrices) != z)
            def _():
                remote(block, block, z_s.at[n], z_r.at[0], x_peer).wait_send()

        summed = part_ref[f]
        for q in range(fs_size - 1):
            part_copy(q).wait()
            summed = summed + landed[q]
        mixed_ref[...] = summed.astype(mixed_ref.dtype)

    pl.when(s == x)(lambda: run(True))
    pl.when(s != x)(lambda: run(False))


def exchanged(tokens, route_experts, route_logits, norm_gain, gate_train, up_train, down_train, fs_size):
    experts, rows, width = gate_train.shape
    count, depth = tokens.shape
    matrices = 3
    total = matrices * PARTS * experts
    units = matrices * experts
    anywhere = pl.BlockSpec(memory_space=pl.ANY)
    in_vmem = pl.BlockSpec(memory_space=pltpu.VMEM)
    dma = pltpu.SemaphoreType.DMA
    return pl.pallas_call(
        exchange_kernel,
        in_specs=[in_vmem] * 4 + [anywhere] * 3,
        out_specs=[in_vmem, anywhere, in_vmem],
        out_shape=[
            pltpu.VMEM((matrices, fs_size * rows, 2 * width), jnp.bfloat16),
            jax.ShapeDtypeStruct((matrices, experts, rows, width), jnp.bfloat16),
            jax.ShapeDtypeStruct((count, depth), jnp.bfloat16),
        ],
        scratch_shapes=[
            pltpu.VMEM((fs_size, count, depth), jnp.float32),
            pltpu.VMEM((fs_size - 1, count, depth), jnp.float32),
            pltpu.VMEM((matrices, experts, rows, width), jnp.bfloat16),
            pltpu.VMEM((SLOTS, rows // PARTS, width), jnp.float32),
            pltpu.VMEM((rows, PAD), jnp.float32),
            pltpu.VMEM((fs_size, count, depth + PAD), jnp.bfloat16),
            pltpu.VMEM((2, fs_size * count, 2 * width), jnp.float32),
            pltpu.VMEM((fs_size * count, 2 * width), jnp.bfloat16),
            dma((SLOTS,)),
            dma((units,)),
            dma((total,)),
            dma((units,)),
            dma((total,)),
            dma((units,)),
            dma((total,)),
            dma((2 * units,)),
            dma((2 * units,)),
            dma((fs_size - 1,)),
            dma((fs_size - 1,)),
            dma((fs_size - 1,)),
            dma((fs_size - 1,)),
            dma((SUB,)),
            dma((SUB,)),
            dma((SUB,)),
        ],
        compiler_params=pltpu.CompilerParams(
            collective_id=0, has_side_effects=True, vmem_limit_bytes=VMEM_LIMIT
        ),
        name="exchange_weights",
    )(tokens, route_experts, route_logits, norm_gain[None, :], gate_train, up_train, down_train)


def store_kernel(joined, gate_ref, up_ref, down_ref, sems):
    piece = joined.shape[1] // STORES
    copies = [
        pltpu.make_async_copy(
            joined.at[m, pl.ds(n * piece, piece)], out.at[0, pl.ds(n * piece, piece)],
            sems.at[m, n],
        )
        for m, out in enumerate((gate_ref, up_ref, down_ref))
        for n in range(STORES)
    ]
    for copy in copies:
        copy.start()
    for copy in copies:
        copy.wait()


def stored(joined):
    matrices, depth, width = joined.shape
    return pl.pallas_call(
        store_kernel,
        in_specs=[pl.BlockSpec(memory_space=pltpu.VMEM)],
        out_specs=[pl.BlockSpec(memory_space=pl.ANY)] * matrices,
        out_shape=[jax.ShapeDtypeStruct((1, depth, width), joined.dtype)] * matrices,
        scratch_shapes=[pltpu.SemaphoreType.DMA((matrices, STORES))],
        compiler_params=pltpu.CompilerParams(vmem_limit_bytes=STORE_LIMIT),
        name="store_weights",
    )(pltpu.with_memory_space_constraint(joined, pltpu.VMEM))


def per_device(tokens, route_experts, route_logits, norm_gain, gate_train, up_train, down_train):
    joined, _, mixed = exchanged(
        tokens, route_experts, route_logits, norm_gain, gate_train, up_train, down_train,
        lax.axis_size("fs"),
    )
    return (*stored(joined), mixed)


def two_by_two(fs_size, tp_size, experts):
    return fs_size == 2 * experts and tp_size == 4 and experts == 4


def choose(*args):
    fits = two_by_two(lax.axis_size("fs"), lax.axis_size("tp"), args[4].shape[0])
    return (per_device if fits else per_device_general)(*args)


def solution(mesh):
    return jax.shard_map(
        choose,
        mesh=mesh,
        in_specs=(
            P(("fs", "tp"), None),
            P(("fs", "tp"), None),
            P(("fs", "tp"), None),
            P("fs"),
            P(None, "fs", "tp"),
            P(None, "fs", "tp"),
            P(None, "fs", "tp"),
        ),
        out_specs=(
            P("fs", None, None),
            P("fs", None, None),
            P("fs", None, None),
            P(("fs", "tp"), None),
        ),
        check_vma=False,
    )
```
